128 devices in a mesh: sp: 16 (over z, x), tp: 8 (over y, core).
Axes of the slice: x: 4, y: 4, z: 4, core: 2. Of those that a mesh axis runs over, the one named last changes fastest.
Arguments:
- stream: bfloat16 [16384, 2048], P(('sp', 'tp')), may hold values from -6 to 6
- projected: bfloat16 [16384, 2048], P('sp', 'tp'), may hold values from -6 to 6
- segments: int32 [16384], P('sp'), may hold values from 0 to 7, never falling along the last dimension, each value on 1 to 3072 neighbouring positions
- group_weight: bfloat16 [4, 512, 512], replicated, may hold values from -0.25 to 0.25
- group_scale: float32 [2048], replicated, may hold values from 0.1 to 1.9
- out_weight: bfloat16 [2048, 2048], replicated, may hold values from -0.125 to 0.125
- ffn_gain: float32 [2048], replicated, may hold values from 0.1 to 1.9
- routes: int32 [16384, 4], P(('sp', 'tp')), may hold values from 0 to 127, all different within a row; in each aligned block of 128 rows (0 to 127, 128 to 255, ...) at most 6 rows name the same one
- route_weights: float32 [16384, 4], P(('sp', 'tp')), may hold values from 0.05 to 0.5
- expert_gate: bfloat16 [128, 2048, 1024], P(('sp', 'tp')), may hold values from -0.25 to 0.25
- expert_up: bfloat16 [128, 2048, 1024], P(('sp', 'tp')), may hold values from -0.25 to 0.25
- expert_down: bfloat16 [128, 1024, 2048], P(('sp', 'tp')), may hold values from -0.1875 to 0.1875
Outputs:
- combined: bfloat16 [16384, 2048], P(('sp', 'tp'))
The draws below stay inside these ranges and needn't reach their ends.
Inputs may be any that keep to these rules, and one draw needn't show every extreme that they name: `segments`: document numbers never fall along the positions; a document has 1 to 3072 positions, and one has exactly 3072. `routes`: each row names 4 different experts. Among the 128 rows of one device (aligned blocks), no expert is named more than 6 times, and in some blocks one is named exactly 6 times.
All inputs are finite; a program needn't handle non-finite values.
Results may differ from the reference program's by a relative error of at most 0.015.
Values may be sent and summed in bfloat16 or wider, within the bound.
A program may use at most 128 MiB of HBM per device.

```python
import math
import jax
import jax.numpy as jnp
import numpy as np
from jax import lax

D = 2048
GROUPS = 4
FF = 1024
TOP = 4
TOK_DEV = 128
TOKENS = 16384
GROUP_WIDTH = 512
EXPERTS = 128
CAP = 6
DOCS = 8
DOC_MOST = 3072


def levels(key, extent, shards, low, high):
    def one(dim, shards_of):
        heights = jax.random.uniform(jax.random.fold_in(jax.random.fold_in(key, 6), dim), (shards_of,), jnp.float32, low / len(shards), high / len(shards))
        return jnp.repeat(jnp.exp(heights), extent[dim] // shards_of).reshape((-1,) + (1,) * (len(extent) - dim - 1))

    loudness = one(*shards[0])
    for cut in shards[1:]:
        loudness = loudness * one(*cut)
    return loudness


def split_up(count, total, bound, skew):
    loads = [(1 << 20) // math.isqrt(standing ** skew) + 1 for standing in range(2, count + 1)]
    rest, given = total - bound - (count - 1), [1] * (count - 1)
    while rest > 0:
        candidates = [i for i in range(count - 1) if given[i] < bound]
        pool, remaining = sum([loads[i] for i in candidates]), rest
        for i in candidates:
            extra = min(bound - given[i], max(1, remaining * loads[i] // pool), rest)
            given[i] = given[i] + extra
            rest = rest - extra
    return np.array([bound] + given)


def ragged_sizes(own_key, number_of, total, most, skew):
    if number_of == 2:
        one = jax.random.randint(own_key, (), max(1, total - most), min(most, total - 1) + 1)
        return jnp.stack([one, total - one])
    lengths = jnp.asarray(split_up(number_of, total, most, skew), jnp.int32)
    couples = (number_of - 1) // 2
    source_of, taker = lengths[1:1 + 2 * couples:2], lengths[2:2 + 2 * couples:2]
    room = jnp.minimum(source_of - 1, most - taker)
    passed = jax.random.randint(jax.random.fold_in(own_key, 1), (couples,), 0, 1 << 20) % (room + 1)
    lengths = lengths.at[1:1 + 2 * couples:2].set(source_of - passed).at[2:2 + 2 * couples:2].set(taker + passed)
    return lengths[jax.random.permutation(jax.random.fold_in(own_key, 2), number_of)]


def deal_out(own_key, own, number, rows, number_of, top, most, lean):
    ranking = jax.random.permutation(own_key, number_of)
    crowded, usual = load_shares(number_of, rows * top, most, lean, True), load_shares(number_of, rows * top, most, lean, False)
    places = jnp.arange(number_of)

    def named(lengths, turn):
        used = int((lengths > 0).sum())
        fixed = max(1, used // 4)
        passed = fixed + (places - fixed + turn * (used - fixed)) % max(1, number_of - fixed)
        return jnp.zeros((number_of,), jnp.int32).at[ranking[jnp.where(places < fixed, places, passed)]].set(jnp.asarray(lengths, jnp.int32))

    lengths = jnp.where(number % 4 == 0, named(crowded, number // 4), named(usual, number - number // 4 - 1))
    mixed = jax.random.permutation(jax.random.fold_in(own, 3), number_of)
    giver, taker = mixed[0:number_of // 2 * 2:2], mixed[1:number_of // 2 * 2:2]
    margin = jnp.minimum(lengths[giver] - 1, most - lengths[taker]) // 2
    margin = jnp.where((giver == ranking[0]) | (taker == ranking[0]) | (lengths[taker] == 0), 0, jnp.maximum(margin, 0))
    passed = jax.random.randint(jax.random.fold_in(own, 4), (number_of // 2,), 0, 1 << 20) % (margin + 1)
    lengths = lengths.at[giver].add(-passed).at[taker].add(passed)
    labels = jnp.searchsorted(jnp.cumsum(lengths), jnp.arange(rows * top), side="right").astype(jnp.int32)
    table = labels.reshape(top, rows).T
    table = table[jax.random.permutation(jax.random.fold_in(own, 1), rows)]
    turn = jax.random.randint(jax.random.fold_in(own, 2), (rows, 1), 0, top)
    return jnp.take_along_axis(table, (jnp.arange(top)[None, :] + turn) % top, axis=1)


def load_shares(count, total, limit, skew, full):
    weights = [(1 << 20) // math.isqrt(rank ** skew) + 1 for rank in range(1, count + 1)]
    largest = limit if full else min(limit, max(-(-total // count), total * weights[0] // sum(weights)))
    least = 1 if total - largest >= count - 1 else 0
    holding, rest = [largest] + [least] * (count - 1), total - largest - least * (count - 1)
    while rest > 0:
        candidates = [i for i in range(1, count) if holding[i] < largest] or [i for i in range(1, count) if holding[i] < limit]
        pool, remaining = sum([weights[i] for i in candidates]), rest
        for i in candidates:
            addition = min(limit - holding[i], max(1, remaining * weights[i] // pool), rest)
            holding[i] = holding[i] + addition
            rest = rest - addition
    return np.array(holding)


def centred(stream_key, dims, spread, limit, cuts=(), kind=jnp.bfloat16):
    entries = spread * jax.random.normal(stream_key, dims, jnp.float32)
    if cuts:
        entries = entries * levels(stream_key, dims, cuts, -0.22, 0.18)
    return jnp.clip(entries, -limit, limit).astype(kind)


def setup_inputs(seed: int = 0) -> dict:
    streams_of = jax.random.split(jax.random.key(seed), 13)
    stream = centred(streams_of[0], (TOKENS, D), 1.0, 6.0, ((0, 128),))
    projected = centred(streams_of[1], (TOKENS, D), 1.0, 6.0, ((0, 16), (1, 8)))
    segments = jnp.searchsorted(jnp.cumsum(ragged_sizes(streams_of[2], DOCS, TOKENS, DOC_MOST, 2)), jnp.arange(TOKENS), side="right").astype(jnp.int32)
    group_weight = centred(streams_of[3], (GROUPS, GROUP_WIDTH, GROUP_WIDTH), GROUP_WIDTH ** -0.5, 0.25)
    group_scale = jnp.clip(1.0 + 0.18 * jax.random.normal(streams_of[4], (D,), jnp.float32), 0.1, 1.9)
    out_weight = centred(streams_of[5], (D, D), D ** -0.5, 0.125)
    ffn_gain = jnp.clip(1.0 + 0.18 * jax.random.normal(streams_of[6], (D,), jnp.float32), 0.1, 1.9)
    routes_keys = jax.random.split(jax.random.fold_in(streams_of[7], 1), TOKENS // TOK_DEV)
    routes_turns = jax.random.permutation(jax.random.fold_in(streams_of[7], 3), TOKENS // TOK_DEV)
    routes = jax.vmap(lambda own, number: deal_out(jax.random.fold_in(streams_of[7], 2), own, number, TOK_DEV, EXPERTS, TOP, CAP, 2))(routes_keys, routes_turns).reshape((TOKENS, TOP))
    route_weights = jnp.clip(0.05 + 0.45 * jax.random.uniform(streams_of[8], (TOKENS, TOP), jnp.float32) ** levels(streams_of[8], (TOKENS, TOP), ((0, 128),), -0.2, 0.2), 0.05, 0.5)
    expert_gate = centred(streams_of[9], (EXPERTS, D, FF), (D // 4) ** -0.5, 0.25, ((0, 128),))
    expert_up = centred(streams_of[10], (EXPERTS, D, FF), (D // 4) ** -0.5, 0.25, ((0, 128),))
    expert_down = centred(streams_of[11], (EXPERTS, FF, D), FF ** -0.5, 0.1875, ((0, 128),))
    return {"stream": stream, "projected": projected, "segments": segments, "group_weight": group_weight, "group_scale": group_scale, "out_weight": out_weight, "ffn_gain": ffn_gain, "routes": routes, "route_weights": route_weights, "expert_gate": expert_gate, "expert_up": expert_up, "expert_down": expert_down}


norm_eps = 1e-05
clamp_limit = 7.0
sigmoid_alpha = 1.702
longest_window = 16

def pool_residue(projected, segments):
    length, channels = projected.shape
    values = projected.astype(jnp.float32)
    channel = jnp.arange(channels, dtype=jnp.int32)
    window = jnp.left_shift(jnp.full((channels,), 2, jnp.int32), channel // (channels // GROUPS))
    window_sum = jnp.zeros((length, channels), jnp.float32)
    window_count = jnp.zeros((length, channels), jnp.float32)
    for offset in range(longest_window):
        earlier_rows = jnp.pad(values, ((offset, 0), (0, 0)))[:length]
        earlier_docs = jnp.pad(segments, (offset, 0), constant_values=-1)[:length]
        included = (earlier_docs == segments)[:, None] & (offset < window)[None, :]
        window_sum = window_sum + jnp.where(included, earlier_rows, jnp.float32(0.0))
        window_count = window_count + included.astype(jnp.float32)
    return (window_sum / window_count - values).astype(jnp.bfloat16)

def rms_scale(resid, gain):
    values = resid.astype(jnp.float32)
    inverse = lax.rsqrt(lax.optimization_barrier(jnp.mean(values * values, -1, keepdims=True)) + norm_eps)
    return (values * inverse * gain.astype(jnp.float32)).astype(jnp.bfloat16)

def run_expert(block, gate_matrix, up_matrix, down_matrix):
    leading = block.shape[:-1]
    flat_rows = block.reshape(-1, block.shape[-1])
    gate_value = jnp.dot(flat_rows, gate_matrix, preferred_element_type=jnp.float32)
    up_value = jnp.dot(flat_rows, up_matrix, preferred_element_type=jnp.float32)
    gated = jnp.minimum(gate_value, clamp_limit)
    linear = jnp.clip(up_value, -clamp_limit, clamp_limit)
    activated = (gated * jax.nn.sigmoid(sigmoid_alpha * gated) * (linear + 1.0)).astype(jnp.bfloat16)
    result = jnp.dot(activated, down_matrix, preferred_element_type=jnp.float32).astype(jnp.bfloat16)
    return result.reshape(leading + (down_matrix.shape[1],))

def reference(stream, projected, segments, group_weight, group_scale, out_weight, ffn_gain, routes, route_weights, expert_gate, expert_up, expert_down):
    mixed = pool_residue(projected, segments)
    length, model_width = mixed.shape
    group_width = model_width // GROUPS
    grouped = jnp.einsum('rgc,gcd->rgd', mixed.reshape(length, GROUPS, group_width).astype(jnp.float32), group_weight.astype(jnp.float32)).reshape(length, model_width)
    scaled = (grouped * group_scale.astype(jnp.float32)).astype(jnp.bfloat16)
    mixer_out = jnp.dot(scaled, out_weight, preferred_element_type=jnp.float32)
    resid = (stream.astype(jnp.float32) + mixer_out).astype(jnp.bfloat16)
    normed = rms_scale(resid, ffn_gain)
    flat_routes = routes.reshape(-1)
    flat_weights = route_weights.reshape(-1)
    token_of = jnp.arange(flat_routes.shape[0], dtype=jnp.int32) // TOP
    most_rows = EXPERTS * CAP

    def one_expert(carry, inputs):
        expert_id, gate_matrix, up_matrix, down_matrix = inputs
        matches = flat_routes == expert_id
        picked = jnp.nonzero(matches, size=most_rows, fill_value=0)[0].astype(jnp.int32)
        live = jnp.arange(most_rows, dtype=jnp.int32) < jnp.sum(matches.astype(jnp.int32))
        tokens_in = token_of[picked]
        expert_out = run_expert(normed[tokens_in], gate_matrix, up_matrix, down_matrix)
        weighting = jnp.where(live, flat_weights[picked], jnp.float32(0.0))
        carry = carry.at[tokens_in].add(expert_out.astype(jnp.float32) * weighting[:, None])
        return (carry, None)
    moe_sum, unused = lax.scan(one_expert, jnp.zeros((length, model_width), jnp.float32), (jnp.arange(EXPERTS, dtype=jnp.int32), expert_gate, expert_up, expert_down))
    return (resid.astype(jnp.float32) + moe_sum).astype(jnp.bfloat16)
```

```python
import jax
import jax.numpy as jnp
from jax import lax
from jax.sharding import PartitionSpec as P
from jax.experimental import pallas as pl
from jax.experimental.pallas import tpu as pltpu

GROUPS = 4


norm_eps = 1e-05
clamp_limit = 7.0
sigmoid_alpha = 1.702
longest_window = 16


def sent_to_all(value, axis):
    devices = lax.axis_size(axis)
    return lax.all_to_all(
        jnp.broadcast_to(value[None], (devices, *value.shape)), axis, 0, 0, tiled=True
    )


def joined_by_halves(pieces, combine):
    while len(jax.tree.leaves(pieces)[0]) > 1:
        pieces = jax.vmap(combine)(
            *(jax.tree.map(lambda part: part[side::2], pieces) for side in (0, 1))
        )
    return jax.tree.map(lambda part: part[0], pieces)


def prefix(value, axis, combine, identity):
    devices, index = (lax.axis_size(axis), lax.axis_index(axis))
    passed = jnp.arange(devices) < index

    def kept(part, zero, own):
        part = jnp.where(
            passed.reshape(-1, *(1 for _ in own.shape)), part, jnp.asarray(zero, own.dtype)
        )
        return part

    pieces = jax.tree.map(lambda part: sent_to_all(part, axis), value)
    return joined_by_halves(jax.tree.map(kept, pieces, identity, value), combine)


def rms_scale(resid, gain):
    values = resid.astype(jnp.float32)
    inverse = lax.rsqrt(jnp.mean(values * values, -1, keepdims=True) + norm_eps)
    return (values * inverse * gain).astype(jnp.bfloat16)


def run_expert(block, gate_matrix, up_matrix, down_matrix):
    leading = block.shape[:-1]
    flat_rows = block.reshape(-1, block.shape[-1])
    gate_value = jnp.dot(flat_rows, gate_matrix, preferred_element_type=jnp.float32)
    up_value = jnp.dot(flat_rows, up_matrix, preferred_element_type=jnp.float32)
    gated = jnp.minimum(gate_value, clamp_limit)
    linear = jnp.clip(up_value, -clamp_limit, clamp_limit)
    activated = (gated * jax.nn.sigmoid(sigmoid_alpha * gated) * (linear + 1.0)).astype(
        jnp.bfloat16
    )
    result = jnp.dot(activated, down_matrix, preferred_element_type=jnp.float32).astype(
        jnp.bfloat16
    )
    return result.reshape(leading + (down_matrix.shape[1],))


def keep_latter(earlier, latter):
    present = latter[1] >= 0
    return (
        jnp.where(present[..., None], latter[0], earlier[0]),
        jnp.where(present, latter[1], earlier[1]),
    )


MESH = pl.DeviceIdType.MESH


def exchange_kernel(count, tp_count, in_ref, out_ref, send_sem, recv_sem, own_sem):
    me = lax.axis_index("sp") * tp_count + lax.axis_index("tp")
    own = pltpu.make_async_copy(in_ref.at[me], out_ref.at[me], own_sem)
    own.start()
    barrier = pltpu.get_barrier_semaphore()

    @pl.loop(1, count)
    def _(step):
        peer = lax.rem(me + step, count)
        pl.semaphore_signal(
            barrier,
            inc=1,
            device_id=(peer // tp_count, lax.rem(peer, tp_count)),
            device_id_type=MESH,
        )

    pl.semaphore_wait(barrier, count - 1)

    @pl.loop(1, count)
    def _(step):
        peer = lax.rem(me + lax.rem(step * 37, count), count)
        pltpu.make_async_remote_copy(
            in_ref.at[peer],
            out_ref.at[me],
            send_sem,
            recv_sem,
            device_id=(peer // tp_count, lax.rem(peer, tp_count)),
            device_id_type=MESH,
        ).start()

    rest = pl.ds(0, count - 1)
    pltpu.make_async_copy(in_ref.at[rest], in_ref.at[rest], send_sem).wait()
    pltpu.make_async_copy(out_ref.at[rest], out_ref.at[rest], recv_sem).wait()
    own.wait()


def exchange(blocks, name, collective_id):
    count = blocks.shape[0]
    return pl.pallas_call(
        lambda *refs: exchange_kernel(count, lax.axis_size("tp"), *refs),
        out_shape=jax.ShapeDtypeStruct(blocks.shape, blocks.dtype),
        in_specs=[pl.BlockSpec(memory_space=pltpu.VMEM)],
        out_specs=pl.BlockSpec(memory_space=pltpu.VMEM),
        scratch_shapes=[pltpu.SemaphoreType.DMA] * 3,
        name=name,
        compiler_params=pltpu.CompilerParams(
            collective_id=collective_id, has_side_effects=True, vmem_limit_bytes=16 << 20
        ),
    )(blocks)


def body(
    stream,
    projected,
    segments,
    group_weight,
    group_scale,
    out_weight,
    ffn_gain,
    routes,
    route_weights,
    expert_gate,
    expert_up,
    expert_down,
):
    row_count, channels = projected.shape
    tp_count = lax.axis_size("tp")
    sp_count = lax.axis_size("sp")
    model_width = channels * tp_count
    group_width = model_width // GROUPS
    rim_rows = longest_window - 1
    channel = lax.axis_index("tp") * channels + jnp.arange(channels, dtype=jnp.int32)
    window = jnp.left_shift(jnp.full((channels,), 2, jnp.int32), channel // group_width)
    identity = (jnp.zeros((rim_rows, channels), jnp.bfloat16), jnp.full((rim_rows,), -1, jnp.int32))
    before_rows, before_docs = prefix(
        (projected[row_count - rim_rows :], segments[row_count - rim_rows :]),
        "sp",
        keep_latter,
        identity,
    )
    extended = jnp.concatenate([before_rows, projected], 0)
    extended_docs = jnp.concatenate([before_docs, segments], 0)
    window_sum = jnp.zeros((row_count, channels), jnp.float32)
    window_count = jnp.zeros((row_count, channels), jnp.float32)
    for offset in range(longest_window):
        earlier_rows = extended[rim_rows - offset : rim_rows - offset + row_count].astype(
            jnp.float32
        )
        earlier_docs = extended_docs[rim_rows - offset : rim_rows - offset + row_count]
        included = (earlier_docs == segments)[:, None] & (offset < window)[None, :]
        window_sum = window_sum + jnp.where(included, earlier_rows, jnp.float32(0.0))
        window_count = window_count + included.astype(jnp.float32)
    mixed = (window_sum / window_count - projected.astype(jnp.float32)).astype(jnp.bfloat16)
    tokens_here = lax.all_to_all(mixed, "tp", split_axis=0, concat_axis=1, tiled=True)
    tok_count = tokens_here.shape[0]
    grouped = jnp.einsum(
        "rgc,gcd->rgd",
        tokens_here.reshape(tok_count, GROUPS, group_width),
        group_weight,
        preferred_element_type=jnp.float32,
    ).reshape(tok_count, model_width)
    scaled = (grouped * group_scale).astype(jnp.bfloat16)
    mixer_out = jnp.dot(scaled, out_weight, preferred_element_type=jnp.float32)
    resid = (stream.astype(jnp.float32) + mixer_out).astype(jnp.bfloat16)
    normed = rms_scale(resid, ffn_gain)
    top_count = routes.shape[1]
    expert_count = sp_count * tp_count
    capacity = 3 * tok_count * top_count // (2 * expert_count)
    flat_routes = routes.reshape(-1)
    onehot = (flat_routes[:, None] == jnp.arange(expert_count, dtype=jnp.int32)[None, :]).astype(
        jnp.int32
    )
    ranking = jnp.sum((jnp.cumsum(onehot, 0) - onehot) * onehot, 1)
    slot_index = flat_routes * capacity + ranking
    token_of = jnp.arange(flat_routes.shape[0], dtype=jnp.int32) // top_count
    slot_token = jnp.zeros((expert_count * capacity,), jnp.int32).at[slot_index].set(token_of)
    slot_live = jnp.zeros((expert_count * capacity,), jnp.bool_).at[slot_index].set(True)
    outgoing = jnp.where(slot_live[:, None], normed[slot_token], jnp.zeros((), jnp.bfloat16))
    arrived = exchange(outgoing.reshape(expert_count, capacity * 8, model_width // 8), "dispatch", 0)
    results = run_expert(
        arrived.reshape(expert_count * capacity, model_width),
        expert_gate[0],
        expert_up[0],
        expert_down[0],
    )
    returned = exchange(results.reshape(expert_count, capacity * 8, model_width // 8), "giveback", 1)
    picked = returned.reshape(expert_count * capacity, model_width)[slot_index]
    weighted = picked.astype(jnp.float32) * route_weights.reshape(-1)[:, None]
    moe_sum = jnp.sum(weighted.reshape(tok_count, top_count, model_width), 1)
    return (resid.astype(jnp.float32) + moe_sum).astype(jnp.bfloat16)


def solution(mesh):
    in_specs = (
        P(("sp", "tp"), None),
        P("sp", "tp"),
        P("sp"),
        P(),
        P(),
        P(),
        P(),
        P(("sp", "tp"), None),
        P(("sp", "tp"), None),
        P(("sp", "tp"), None, None),
        P(("sp", "tp"), None, None),
        P(("sp", "tp"), None, None),
    )
    out_specs = P(("sp", "tp"), None)
    return jax.shard_map(body, mesh=mesh, in_specs=in_specs, out_specs=out_specs, check_vma=False)
```

```python
import functools

import jax
import jax.numpy as jnp
from jax import lax
from jax.experimental import pallas as pl
from jax.experimental.pallas import tpu as pltpu
from jax.sharding import PartitionSpec as P

GROUPS = 4
CAPACITY = 6
STRIDE = 37
INVERSE = 45
PARTS = 8
BATCH = 16
FIRST_WINDOW = 2

norm_eps = 1e-05
clamp_limit = 7.0
sigmoid_alpha = 1.702
MESH = pl.DeviceIdType.MESH
F32 = jnp.float32
BF16 = jnp.bfloat16


def iota(shape, axis):
    return lax.broadcasted_iota(jnp.int32, shape, axis)


def quotient(value, divisor):
    return jnp.floor((value.astype(F32) + 0.5) * (1.0 / divisor))


def dot(left, right):
    return jnp.dot(left, right, preferred_element_type=F32)


def layer_kernel(
    stream_hbm,
    projected_hbm,
    segments_hbm,
    group_hbm,
    scale_hbm,
    out_weight_hbm,
    gain_hbm,
    routes_hbm,
    weights_hbm,
    gate_hbm,
    up_hbm,
    down_hbm,
    combined_ref,
    stream_ref,
    extended,
    segments_ref,
    segments_before,
    group_ref,
    scale_ref,
    out_weight_ref,
    gain_ref,
    routes_ref,
    weights_ref,
    gate_ref,
    up_ref,
    down_ref,
    mixed_out,
    mixed_in,
    total,
    resid_ref,
    normed_ref,
    unpack_ref,
    pack_ref,
    rank_ref,
    rank_turned,
    share_turned,
    wide_ref,
    tall_ref,
    hidden_ref,
    sent,
    arrived,
    results,
    returned,
    load_sems,
    halo_sems,
    mixed_sends,
    mixed_recvs,
    sent_sem,
    arrived_sems,
    results_sem,
    returned_sems,
):
    sp_count, tp_count = lax.axis_size("sp"), lax.axis_size("tp")
    count = sp_count * tp_count
    sp, tp = lax.axis_index("sp"), lax.axis_index("tp")
    me = sp * tp_count + tp
    tokens, width = stream_ref.shape
    channels = width // tp_count
    group_width = width // GROUPS
    batches = count // BATCH
    rows = BATCH * CAPACITY
    piece = width // PARTS
    packed_rows = rows * PARTS
    message = CAPACITY * PARTS

    def device(index):
        return (index // tp_count, lax.rem(index, tp_count))

    loads = [
        pltpu.make_async_copy(source, target, load_sems.at[number])
        for number, (source, target) in enumerate(
            [
                (projected_hbm, extended.at[pl.ds(tokens, tokens * tp_count)]),
                (segments_hbm, segments_ref),
                (routes_hbm, routes_ref),
                (weights_hbm, weights_ref),
                (group_hbm, group_ref),
                (out_weight_hbm, out_weight_ref),
                (scale_hbm, scale_ref),
                (stream_hbm, stream_ref),
                (gain_hbm, gain_ref),
                (gate_hbm, gate_ref),
                (up_hbm, up_ref),
                (down_hbm, down_ref),
            ]
        )
    ]
    for load in loads:
        load.start()

    barrier = pltpu.get_barrier_semaphore()

    @pl.loop(1, count)
    def _(step):
        pl.semaphore_signal(
            barrier, inc=1, device_id=device(lax.rem(me + step, count)), device_id_type=MESH
        )

    window = jnp.left_shift(FIRST_WINDOW, tp // (tp_count // GROUPS))
    extended[pl.ds(0, tokens - 16), :] = jnp.zeros((tokens - 16, channels), BF16)
    for load in loads[:2]:
        load.wait()
    back = tokens + iota((tokens, 2 * tokens), 0) - iota((tokens, 2 * tokens), 1)
    in_window = (back >= 0) & (back < window)

    def pool(block, docs_before):
        docs = segments_ref[block : block + 1, :]
        docs_there = jnp.concatenate([docs_before, docs], axis=1).astype(F32)
        docs_here = jnp.broadcast_to(docs.astype(F32), (tokens, tokens)).T
        docs_here = jnp.concatenate([docs_here, docs_here], axis=1)
        included = jnp.where(in_window & (docs_here == docs_there), 1.0, 0.0).astype(BF16)
        sums = dot(included, extended[pl.ds(block * tokens, 2 * tokens), :])
        counts = dot(included, jnp.ones((2 * tokens, channels), BF16))
        own = extended[pl.ds((block + 1) * tokens, tokens), :].astype(F32)
        mixed_out[block] = (sums / counts - own).astype(BF16)

    for block in range(1, tp_count):
        pool(block, segments_ref[block - 1 : block, :])

    for load in loads[2:4]:
        load.wait()
    order = jnp.bitwise_and((routes_ref[...] - me) * INVERSE, count - 1)
    square = (count, tokens)
    chosen = jnp.zeros(square, F32)
    share = jnp.zeros(square, F32)
    for choice in range(routes_ref.shape[0]):
        match = iota(square, 0) == order[choice : choice + 1, :]
        chosen = chosen + jnp.where(match, 1.0, 0.0)
        share = share + jnp.where(match, weights_ref[choice : choice + 1, :], 0.0)
    earlier = jnp.where(iota((tokens, tokens), 0) < iota((tokens, tokens), 1), 1.0, 0.0)
    rank = jnp.where(chosen > 0.0, dot(chosen.astype(BF16), earlier.astype(BF16)), -1.0)
    rank_ref[...] = rank.astype(BF16)
    rank_turned[...] = rank.T.astype(BF16)
    share = share.T
    share_high = share.astype(BF16)
    share_turned[0] = share_high
    share_turned[1] = (share - share_high.astype(F32)).astype(BF16)

    turned = (packed_rows, packed_rows)

    def message_row(value):
        part = quotient(value, rows)
        within = value.astype(F32) - part * rows
        peer = quotient(within, CAPACITY)
        return peer * message + part * CAPACITY + (within - peer * CAPACITY)

    unpack_ref[...] = jnp.where(
        message_row(iota((packed_rows, 1), 0)) == iota(turned, 1).astype(F32), 1.0, 0.0
    ).astype(BF16)
    pack_ref[...] = jnp.where(
        message_row(iota((1, packed_rows), 1)) == iota(turned, 0).astype(F32), 1.0, 0.0
    ).astype(BF16)

    def packed():
        return dot(pack_ref[...], tall_ref[...]).astype(BF16).reshape(BATCH, message, piece)

    def unpack(block):
        tall = dot(unpack_ref[...], block.reshape(packed_rows, piece)).astype(BF16)
        for part in range(PARTS):
            wide_ref[:, part * piece : (part + 1) * piece] = tall[part * rows : (part + 1) * rows]

    pl.semaphore_wait(barrier, count - 1)

    following = (lax.rem(sp + 1, sp_count), tp)
    halo = [
        pltpu.make_async_remote_copy(
            extended.at[pl.ds(tokens * (tp_count + 1) - 16, 16)],
            extended.at[pl.ds(tokens - 16, 16)],
            halo_sems.at[0],
            halo_sems.at[1],
            device_id=following,
            device_id_type=MESH,
        ),
        pltpu.make_async_remote_copy(
            segments_ref,
            segments_before,
            halo_sems.at[2],
            halo_sems.at[3],
            device_id=following,
            device_id_type=MESH,
        ),
    ]
    for copy in halo:
        copy.start()

    def mixed_copy(peer):
        return pltpu.make_async_remote_copy(
            mixed_out.at[peer],
            mixed_in.at[tp],
            mixed_sends.at[peer],
            mixed_recvs.at[tp],
            device_id=(sp, peer),
            device_id_type=MESH,
        )

    for step in range(1, tp_count):
        peer = lax.rem(tp + step, tp_count)

        @pl.when(peer != 0)
        def _():
            mixed_copy(peer).start()

    for copy in halo:
        copy.wait()
    docs_before = jnp.where(sp > 0, segments_before[tp_count - 1 : tp_count, :], -1)
    pool(0, docs_before)

    @pl.when(tp != 0)
    def _():
        mixed_copy(0).start()

    mixed_in[tp] = mixed_out[tp]

    for load in loads[4:9]:
        load.wait()
    total[...] = stream_ref[...].astype(F32)
    for step in (0, 1, 3, 2):
        per_group = tp_count // GROUPS
        group = lax.rem(tp // per_group + step, GROUPS)
        grouped = jnp.zeros((tokens, group_width), F32)
        for member in range(per_group):
            source = group * per_group + member

            @pl.when(source != tp)
            def _():
                block = mixed_in.at[source]
                pltpu.make_async_copy(block, block, mixed_recvs.at[source]).wait()

            grouped = grouped + dot(
                mixed_in[source], group_ref[group, member * channels : (member + 1) * channels, :]
            )
        scale = scale_ref[:, pl.ds(pl.multiple_of(group * group_width, group_width), group_width)]
        total[...] += dot((grouped * scale).astype(BF16), out_weight_ref[group])

    resid = total[...].astype(BF16)
    resid_ref[...] = resid
    values = resid.astype(F32)
    inverse = lax.rsqrt(jnp.mean(values * values, -1, keepdims=True) + norm_eps)
    normed_ref[...] = (values * inverse * gain_ref[...]).astype(BF16)

    @pl.loop(0, batches)
    def _(batch):
        names = (batch * BATCH).astype(F32) + quotient(iota((rows, count), 0), CAPACITY)
        slot = iota((rows, 1), 0).astype(F32) - CAPACITY * quotient(iota((rows, 1), 0), CAPACITY)
        spread = jnp.where(names == iota((rows, count), 1).astype(F32), 1.0, 0.0).astype(BF16)
        select = jnp.where(dot(spread, rank_ref[...]) == slot, 1.0, 0.0).astype(BF16)
        for part in range(PARTS):
            tall_ref[part * rows : (part + 1) * rows, :] = dot(
                select, normed_ref[:, part * piece : (part + 1) * piece]
            ).astype(BF16)
        sent[pl.ds(batch * BATCH, BATCH)] = packed()

        @pl.when(batch == 0)
        def _():
            arrived[0] = sent[0]

        @pl.loop(jnp.where(batch == 0, 1, 0), BATCH)
        def _(step):
            name = batch * BATCH + step
            pltpu.make_async_remote_copy(
                sent.at[name],
                arrived.at[name],
                sent_sem,
                arrived_sems.at[batch],
                device_id=device(lax.rem(me + name * STRIDE, count)),
                device_id_type=MESH,
            ).start()

    def wait_batch(buffer, sems, batch):
        @pl.when(batch == 0)
        def _():
            part = buffer.at[pl.ds(1, BATCH - 1)]
            pltpu.make_async_copy(part, part, sems.at[0]).wait()

        @pl.when(batch != 0)
        def _():
            part = buffer.at[pl.ds(batch * BATCH, BATCH)]
            pltpu.make_async_copy(part, part, sems.at[batch]).wait()

    for load in loads[9:]:
        load.wait()

    @pl.loop(0, batches)
    def _(batch):
        wait_batch(arrived, arrived_sems, batch)
        unpack(arrived[pl.ds(batch * BATCH, BATCH)])
        block = wide_ref[...]
        hidden = hidden_ref.shape[1]
        for start in range(0, hidden, 256):
            columns = slice(start, start + 256)
            gated = jnp.minimum(dot(block, gate_ref[0, :, columns]), clamp_limit)
            linear = jnp.clip(dot(block, up_ref[0, :, columns]), -clamp_limit, clamp_limit)
            hidden_ref[:, columns] = (
                gated * jax.nn.sigmoid(sigmoid_alpha * gated) * (linear + 1.0)
            ).astype(BF16)
        for part in range(PARTS):
            tall_ref[part * rows : (part + 1) * rows, :] = dot(
                hidden_ref[...], down_ref[0, :, part * piece : (part + 1) * piece]
            ).astype(BF16)
        results[pl.ds(batch * BATCH, BATCH)] = packed()

        @pl.when(batch == 0)
        def _():
            returned[0] = results[0]

        @pl.loop(jnp.where(batch == 0, 1, 0), BATCH)
        def _(step):
            name = batch * BATCH + step
            pltpu.make_async_remote_copy(
                results.at[name],
                returned.at[name],
                results_sem,
                returned_sems.at[batch],
                device_id=device(lax.rem(me + (count - name) * STRIDE, count)),
                device_id_type=MESH,
            ).start()

    total[...] = resid_ref[...].astype(F32)

    @pl.loop(0, batches)
    def _(batch):
        names = (batch * BATCH).astype(F32) + quotient(iota((count, rows), 1), CAPACITY)
        slot = iota((1, rows), 1).astype(F32) - CAPACITY * quotient(iota((1, rows), 1), CAPACITY)
        spread = jnp.where(names == iota((count, rows), 0).astype(F32), 1.0, 0.0).astype(BF16)
        live = dot(rank_turned[...], spread) == slot
        high = jnp.where(live, dot(share_turned[0], spread), 0.0).astype(BF16)
        low = jnp.where(live, dot(share_turned[1], spread), 0.0).astype(BF16)
        wait_batch(returned, returned_sems, batch)
        unpack(returned[pl.ds(batch * BATCH, BATCH)])
        total[...] += dot(high, wide_ref[...]) + dot(low, wide_ref[...])

    combined_ref[...] = total[...].astype(BF16)

    for step in range(1, tp_count):
        mixed_copy(lax.rem(tp + step, tp_count)).wait_send()
    rest = pl.ds(1, count - 1)
    pltpu.make_async_copy(sent.at[rest], sent.at[rest], sent_sem).wait()
    pltpu.make_async_copy(results.at[rest], results.at[rest], results_sem).wait()


def body(
    stream,
    projected,
    segments,
    group_weight,
    group_scale,
    out_weight,
    ffn_gain,
    routes,
    route_weights,
    expert_gate,
    expert_up,
    expert_down,
):
    tokens, width = stream.shape
    tp_count = lax.axis_size("tp")
    count = lax.axis_size("sp") * tp_count
    channels = width // tp_count
    hidden = expert_gate.shape[2]
    rows = BATCH * CAPACITY
    piece = width // PARTS
    operands = (
        stream,
        projected,
        segments.reshape(-1, tokens),
        group_weight,
        group_scale.reshape(1, -1),
        out_weight.reshape(GROUPS, width // GROUPS, width),
        ffn_gain.reshape(1, -1),
        routes.T,
        route_weights.T,
        expert_gate,
        expert_up,
        expert_down,
    )
    messages = (count, CAPACITY * PARTS, piece)
    batches = count // BATCH
    vmem = pltpu.VMEM
    dma = pltpu.SemaphoreType.DMA
    return pl.pallas_call(
        layer_kernel,
        out_shape=jax.ShapeDtypeStruct((tokens, width), BF16),
        in_specs=[pl.BlockSpec(memory_space=pl.ANY)] * len(operands),
        out_specs=pl.BlockSpec(memory_space=pltpu.VMEM),
        scratch_shapes=[
            vmem((tokens, width), BF16),
            vmem((tokens * (tp_count + 1), channels), BF16),
            vmem((tp_count, tokens), jnp.int32),
            vmem((tp_count, tokens), jnp.int32),
            vmem(group_weight.shape, BF16),
            vmem((1, width), F32),
            vmem((GROUPS, width // GROUPS, width), BF16),
            vmem((1, width), F32),
            vmem(routes.shape[::-1], jnp.int32),
            vmem(routes.shape[::-1], F32),
            vmem(expert_gate.shape, BF16),
            vmem(expert_up.shape, BF16),
            vmem(expert_down.shape, BF16),
            vmem((tp_count, tokens, channels), BF16),
            vmem((tp_count, tokens, channels), BF16),
            vmem((tokens, width), F32),
            vmem((tokens, width), BF16),
            vmem((tokens, width), BF16),
            vmem((rows * PARTS, rows * PARTS), BF16),
            vmem((rows * PARTS, rows * PARTS), BF16),
            vmem((count, tokens), BF16),
            vmem((tokens, count), BF16),
            vmem((2, tokens, count), BF16),
            vmem((rows, width), BF16),
            vmem((rows * PARTS, piece), BF16),
            vmem((rows, hidden), BF16),
            vmem(messages, BF16),
            vmem(messages, BF16),
            vmem(messages, BF16),
            vmem(messages, BF16),
            dma((len(operands),)),
            dma((4,)),
            dma((tp_count,)),
            dma((tp_count,)),
            dma,
            dma((batches,)),
            dma,
            dma((batches,)),
        ],
        name="layer",
        compiler_params=pltpu.CompilerParams(
            collective_id=0, has_side_effects=True, vmem_limit_bytes=60 << 20
        ),
    )(*operands)


def solution(mesh):
    in_specs = (
        P(("sp", "tp"), None),
        P("sp", "tp"),
        P("sp"),
        P(),
        P(),
        P(),
        P(),
        P(("sp", "tp"), None),
        P(("sp", "tp"), None),
        P(("sp", "tp"), None, None),
        P(("sp", "tp"), None, None),
        P(("sp", "tp"), None, None),
    )
    out_specs = P(("sp", "tp"), None)
    return jax.shard_map(body, mesh=mesh, in_specs=in_specs, out_specs=out_specs, check_vma=False)
```

```python
import functools

import jax
import jax.numpy as jnp
from jax import lax
from jax.experimental import pallas as pl
from jax.experimental.pallas import tpu as pltpu
from jax.sharding import PartitionSpec as P

GROUPS = 4
CAPACITY = 6
STRIDE = 37
INVERSE = 45
PARTS = 8
BATCH = 16
FIRST_WINDOW = 2

norm_eps = 1e-05
clamp_limit = 7.0
sigmoid_alpha = 1.702
MESH = pl.DeviceIdType.MESH
F32 = jnp.float32
BF16 = jnp.bfloat16


def iota(shape, axis):
    return lax.broadcasted_iota(jnp.int32, shape, axis)


def quotient(value, divisor):
    return jnp.floor((value.astype(F32) + 0.5) * (1.0 / divisor))


def dot(left, right):
    return jnp.dot(left, right, preferred_element_type=F32)


def layer_kernel(
    stream_hbm,
    projected_hbm,
    segments_hbm,
    group_hbm,
    scale_hbm,
    out_weight_hbm,
    gain_hbm,
    routes_hbm,
    weights_hbm,
    gate_hbm,
    up_hbm,
    down_hbm,
    combined_ref,
    stream_ref,
    extended,
    segments_ref,
    segments_before,
    group_ref,
    scale_ref,
    out_weight_ref,
    gain_ref,
    routes_ref,
    weights_ref,
    gate_ref,
    up_ref,
    down_ref,
    mixed_out,
    mixed_in,
    total,
    resid_ref,
    normed_ref,
    unpack_ref,
    pack_ref,
    rank_ref,
    rank_turned,
    share_turned,
    picks,
    wide_ref,
    tall_ref,
    hidden_ref,
    sent,
    arrived,
    results,
    returned,
    load_sems,
    halo_sems,
    mixed_sends,
    mixed_recvs,
    sent_sem,
    arrived_sems,
    results_sem,
    returned_sems,
    ready,
):
    sp_count, tp_count = lax.axis_size("sp"), lax.axis_size("tp")
    count = sp_count * tp_count
    sp, tp = lax.axis_index("sp"), lax.axis_index("tp")
    me = sp * tp_count + tp
    tokens, width = stream_ref.shape
    channels = width // tp_count
    group_width = width // GROUPS
    batches = count // BATCH
    rows = BATCH * CAPACITY
    piece = width // PARTS
    packed_rows = rows * PARTS
    message = CAPACITY * PARTS

    def device(index):
        return (index // tp_count, lax.rem(index, tp_count))

    loads = [
        pltpu.make_async_copy(source, target, load_sems.at[number])
        for number, (source, target) in enumerate(
            [
                (projected_hbm, extended.at[pl.ds(tokens, tokens * tp_count)]),
                (segments_hbm, segments_ref),
                (routes_hbm, routes_ref),
                (weights_hbm, weights_ref),
                (group_hbm, group_ref),
                (out_weight_hbm, out_weight_ref),
                (scale_hbm, scale_ref),
                (stream_hbm, stream_ref),
                (gain_hbm, gain_ref),
                (gate_hbm, gate_ref),
                (up_hbm, up_ref),
                (down_hbm, down_ref),
            ]
        )
    ]
    for load in loads:
        load.start()

    barrier = pltpu.get_barrier_semaphore()

    for step in range(1, tp_count):
        pl.semaphore_signal(
            barrier,
            inc=1,
            device_id=(sp, lax.rem(tp + step, tp_count)),
            device_id_type=MESH,
        )
    for step in range(1, sp_count):
        pl.semaphore_signal(
            barrier,
            inc=1,
            device_id=(lax.rem(sp + step, sp_count), tp),
            device_id_type=MESH,
        )

    turned = (packed_rows, packed_rows)

    def message_row(value):
        part = quotient(value, rows)
        within = value.astype(F32) - part * rows
        peer = quotient(within, CAPACITY)
        return peer * message + part * CAPACITY + (within - peer * CAPACITY)

    unpack_ref[...] = jnp.where(
        message_row(iota((packed_rows, 1), 0)) == iota(turned, 1).astype(F32), 1.0, 0.0
    ).astype(BF16)
    pack_ref[...] = jnp.where(
        message_row(iota((1, packed_rows), 1)) == iota(turned, 0).astype(F32), 1.0, 0.0
    ).astype(BF16)

    window = jnp.left_shift(FIRST_WINDOW, tp // (tp_count // GROUPS))
    extended[pl.ds(0, tokens - 16), :] = jnp.zeros((tokens - 16, channels), BF16)
    for load in loads[:2]:
        load.wait()
    back = tokens + iota((tokens, 2 * tokens), 0) - iota((tokens, 2 * tokens), 1)
    in_window = (back >= 0) & (back < window)

    def pool(block, docs_before):
        docs = segments_ref[block : block + 1, :]
        docs_there = jnp.concatenate([docs_before, docs], axis=1).astype(F32)
        docs_here = jnp.broadcast_to(docs.astype(F32), (tokens, tokens)).T
        docs_here = jnp.concatenate([docs_here, docs_here], axis=1)
        included = jnp.where(in_window & (docs_here == docs_there), 1.0, 0.0).astype(BF16)
        sums = dot(included, extended[pl.ds(block * tokens, 2 * tokens), :])
        counts = dot(included, jnp.ones((2 * tokens, channels), BF16))
        own = extended[pl.ds((block + 1) * tokens, tokens), :].astype(F32)
        mixed_out[block] = (sums / counts - own).astype(BF16)

    for block in range(1, tp_count):
        pool(block, segments_ref[block - 1 : block, :])

    pl.semaphore_wait(barrier, sp_count + tp_count - 2)

    following = (lax.rem(sp + 1, sp_count), tp)
    halo = [
        pltpu.make_async_remote_copy(
            extended.at[pl.ds(tokens * (tp_count + 1) - 16, 16)],
            extended.at[pl.ds(tokens - 16, 16)],
            halo_sems.at[0],
            halo_sems.at[1],
            device_id=following,
            device_id_type=MESH,
        ),
        pltpu.make_async_remote_copy(
            segments_ref,
            segments_before,
            halo_sems.at[2],
            halo_sems.at[3],
            device_id=following,
            device_id_type=MESH,
        ),
    ]
    for copy in halo:
        copy.start()

    def mixed_copy(peer):
        return pltpu.make_async_remote_copy(
            mixed_out.at[peer],
            mixed_in.at[tp],
            mixed_sends.at[peer],
            mixed_recvs.at[tp],
            device_id=(sp, peer),
            device_id_type=MESH,
        )

    for step in range(1, tp_count):
        peer = lax.rem(tp + step, tp_count)

        @pl.when(peer != 0)
        def _():
            mixed_copy(peer).start()

    for step in range(1, sp_count):
        pl.semaphore_signal(
            ready, inc=1, device_id=(lax.rem(sp + step, sp_count), tp), device_id_type=MESH
        )

    def packed():
        return dot(pack_ref[...], tall_ref[...]).astype(BF16).reshape(BATCH, message, piece)

    def unpack(block):
        tall = dot(unpack_ref[...], block.reshape(packed_rows, piece)).astype(BF16)
        for part in range(PARTS):
            wide_ref[:, part * piece : (part + 1) * piece] = tall[part * rows : (part + 1) * rows]

    for load in loads[2:4]:
        load.wait()
    order = jnp.bitwise_and((routes_ref[...] - me) * INVERSE, count - 1)
    square = (count, tokens)
    chosen = jnp.zeros(square, F32)
    share = jnp.zeros(square, F32)
    for choice in range(routes_ref.shape[0]):
        match = iota(square, 0) == order[choice : choice + 1, :]
        chosen = chosen + jnp.where(match, 1.0, 0.0)
        share = share + jnp.where(match, weights_ref[choice : choice + 1, :], 0.0)
    earlier = jnp.where(iota((tokens, tokens), 0) < iota((tokens, tokens), 1), 1.0, 0.0)
    rank = jnp.where(chosen > 0.0, dot(chosen.astype(BF16), earlier.astype(BF16)), -1.0)
    rank_ref[...] = rank.astype(BF16)
    rank_turned[...] = rank.T.astype(BF16)

    @pl.loop(0, batches)
    def _(batch):
        names = (batch * BATCH).astype(F32) + quotient(iota((rows, count), 0), CAPACITY)
        slot = iota((rows, 1), 0).astype(F32) - CAPACITY * quotient(iota((rows, 1), 0), CAPACITY)
        spread = jnp.where(names == iota((rows, count), 1).astype(F32), 1.0, 0.0).astype(BF16)
        picks[batch] = jnp.where(dot(spread, rank_ref[...]) == slot, 1.0, 0.0).astype(BF16)

    share = share.T
    share_high = share.astype(BF16)
    share_turned[0] = share_high
    share_turned[1] = (share - share_high.astype(F32)).astype(BF16)

    for copy in halo:
        copy.wait()
    docs_before = jnp.where(sp > 0, segments_before[tp_count - 1 : tp_count, :], -1)
    pool(0, docs_before)

    @pl.when(tp != 0)
    def _():
        mixed_copy(0).start()

    mixed_in[tp] = mixed_out[tp]

    for load in loads[4:9]:
        load.wait()
    total[...] = stream_ref[...].astype(F32)
    for step in (0, 1, 3, 2):
        per_group = tp_count // GROUPS
        group = lax.rem(tp // per_group + step, GROUPS)
        grouped = jnp.zeros((tokens, group_width), F32)
        for member in range(per_group):
            source = group * per_group + member

            @pl.when(source != tp)
            def _():
                block = mixed_in.at[source]
                pltpu.make_async_copy(block, block, mixed_recvs.at[source]).wait()

            grouped = grouped + dot(
                mixed_in[source], group_ref[group, member * channels : (member + 1) * channels, :]
            )
        scale = scale_ref[:, pl.ds(pl.multiple_of(group * group_width, group_width), group_width)]
        total[...] += dot((grouped * scale).astype(BF16), out_weight_ref[group])

    resid = total[...].astype(BF16)
    resid_ref[...] = resid
    values = resid.astype(F32)
    inverse = lax.rsqrt(jnp.mean(values * values, -1, keepdims=True) + norm_eps)
    normed_ref[...] = (values * inverse * gain_ref[...]).astype(BF16)

    pl.semaphore_wait(ready, sp_count - 1)

    @pl.loop(0, batches)
    def _(batch):
        select = picks[batch]
        for part in range(PARTS):
            tall_ref[part * rows : (part + 1) * rows, :] = dot(
                select, normed_ref[:, part * piece : (part + 1) * piece]
            ).astype(BF16)
        sent[pl.ds(batch * BATCH, BATCH)] = packed()

        @pl.when(batch == 0)
        def _():
            arrived[0] = sent[0]

        @pl.loop(jnp.where(batch == 0, 1, 0), BATCH)
        def _(step):
            name = batch * BATCH + step
            pltpu.make_async_remote_copy(
                sent.at[name],
                arrived.at[name],
                sent_sem,
                arrived_sems.at[batch],
                device_id=device(lax.rem(me + name * STRIDE, count)),
                device_id_type=MESH,
            ).start()

    def wait_batch(buffer, sems, batch):
        @pl.when(batch == 0)
        def _():
            part = buffer.at[pl.ds(1, BATCH - 1)]
            pltpu.make_async_copy(part, part, sems.at[0]).wait()

        @pl.when(batch != 0)
        def _():
            part = buffer.at[pl.ds(batch * BATCH, BATCH)]
            pltpu.make_async_copy(part, part, sems.at[batch]).wait()

    for load in loads[9:]:
        load.wait()

    @pl.loop(0, batches)
    def _(batch):
        wait_batch(arrived, arrived_sems, batch)
        unpack(arrived[pl.ds(batch * BATCH, BATCH)])
        block = wide_ref[...]
        hidden = hidden_ref.shape[1]
        for start in range(0, hidden, 256):
            columns = slice(start, start + 256)
            gated = jnp.minimum(dot(block, gate_ref[0, :, columns]), clamp_limit)
            linear = jnp.clip(dot(block, up_ref[0, :, columns]), -clamp_limit, clamp_limit)
            hidden_ref[:, columns] = (
                gated * jax.nn.sigmoid(sigmoid_alpha * gated) * (linear + 1.0)
            ).astype(BF16)
        for part in range(PARTS):
            tall_ref[part * rows : (part + 1) * rows, :] = dot(
                hidden_ref[...], down_ref[0, :, part * piece : (part + 1) * piece]
            ).astype(BF16)
        results[pl.ds(batch * BATCH, BATCH)] = packed()

        @pl.when(batch == 0)
        def _():
            returned[0] = results[0]

        @pl.loop(jnp.where(batch == 0, 1, 0), BATCH)
        def _(step):
            name = batch * BATCH + step
            pltpu.make_async_remote_copy(
                results.at[name],
                returned.at[name],
                results_sem,
                returned_sems.at[batch],
                device_id=device(lax.rem(me + (count - name) * STRIDE, count)),
                device_id_type=MESH,
            ).start()

    total[...] = resid_ref[...].astype(F32)

    @pl.loop(0, batches)
    def _(batch):
        names = (batch * BATCH).astype(F32) + quotient(iota((count, rows), 1), CAPACITY)
        slot = iota((1, rows), 1).astype(F32) - CAPACITY * quotient(iota((1, rows), 1), CAPACITY)
        spread = jnp.where(names == iota((count, rows), 0).astype(F32), 1.0, 0.0).astype(BF16)
        live = dot(rank_turned[...], spread) == slot
        high = jnp.where(live, dot(share_turned[0], spread), 0.0).astype(BF16)
        low = jnp.where(live, dot(share_turned[1], spread), 0.0).astype(BF16)
        wait_batch(returned, returned_sems, batch)
        unpack(returned[pl.ds(batch * BATCH, BATCH)])
        total[...] += dot(high, wide_ref[...]) + dot(low, wide_ref[...])

    combined_ref[...] = total[...].astype(BF16)

    for step in range(1, tp_count):
        mixed_copy(lax.rem(tp + step, tp_count)).wait_send()
    rest = pl.ds(1, count - 1)
    pltpu.make_async_copy(sent.at[rest], sent.at[rest], sent_sem).wait()
    pltpu.make_async_copy(results.at[rest], results.at[rest], results_sem).wait()


def body(
    stream,
    projected,
    segments,
    group_weight,
    group_scale,
    out_weight,
    ffn_gain,
    routes,
    route_weights,
    expert_gate,
    expert_up,
    expert_down,
):
    tokens, width = stream.shape
    tp_count = lax.axis_size("tp")
    count = lax.axis_size("sp") * tp_count
    channels = width // tp_count
    hidden = expert_gate.shape[2]
    rows = BATCH * CAPACITY
    piece = width // PARTS
    operands = (
        stream,
        projected,
        segments.reshape(-1, tokens),
        group_weight,
        group_scale.reshape(1, -1),
        out_weight.reshape(GROUPS, width // GROUPS, width),
        ffn_gain.reshape(1, -1),
        routes.T,
        route_weights.T,
        expert_gate,
        expert_up,
        expert_down,
    )
    messages = (count, CAPACITY * PARTS, piece)
    batches = count // BATCH
    vmem = pltpu.VMEM
    dma = pltpu.SemaphoreType.DMA
    return pl.pallas_call(
        layer_kernel,
        out_shape=jax.ShapeDtypeStruct((tokens, width), BF16),
        in_specs=[pl.BlockSpec(memory_space=pltpu.MemorySpace.HBM)] * len(operands),
        out_specs=pl.BlockSpec(memory_space=pltpu.VMEM),
        scratch_shapes=[
            vmem((tokens, width), BF16),
            vmem((tokens * (tp_count + 1), channels), BF16),
            vmem((tp_count, tokens), jnp.int32),
            vmem((tp_count, tokens), jnp.int32),
            vmem(group_weight.shape, BF16),
            vmem((1, width), F32),
            vmem((GROUPS, width // GROUPS, width), BF16),
            vmem((1, width), F32),
            vmem(routes.shape[::-1], jnp.int32),
            vmem(routes.shape[::-1], F32),
            vmem(expert_gate.shape, BF16),
            vmem(expert_up.shape, BF16),
            vmem(expert_down.shape, BF16),
            vmem((tp_count, tokens, channels), BF16),
            vmem((tp_count, tokens, channels), BF16),
            vmem((tokens, width), F32),
            vmem((tokens, width), BF16),
            vmem((tokens, width), BF16),
            vmem((rows * PARTS, rows * PARTS), BF16),
            vmem((rows * PARTS, rows * PARTS), BF16),
            vmem((count, tokens), BF16),
            vmem((tokens, count), BF16),
            vmem((2, tokens, count), BF16),
            vmem((batches, rows, tokens), BF16),
            vmem((rows, width), BF16),
            vmem((rows * PARTS, piece), BF16),
            vmem((rows, hidden), BF16),
            vmem(messages, BF16),
            vmem(messages, BF16),
            vmem(messages, BF16),
            vmem(messages, BF16),
            dma((len(operands),)),
            dma((4,)),
            dma((tp_count,)),
            dma((tp_count,)),
            dma,
            dma((batches,)),
            dma,
            dma((batches,)),
            pltpu.SemaphoreType.REGULAR,
        ],
        name="layer",
        compiler_params=pltpu.CompilerParams(
            collective_id=0, has_side_effects=True, vmem_limit_bytes=50 << 20
        ),
    )(*(pltpu.with_memory_space_constraint(operand, pltpu.MemorySpace.HBM) for operand in operands))


def solution(mesh):
    in_specs = (
        P(("sp", "tp"), None),
        P("sp", "tp"),
        P("sp"),
        P(),
        P(),
        P(),
        P(),
        P(("sp", "tp"), None),
        P(("sp", "tp"), None),
        P(("sp", "tp"), None, None),
        P(("sp", "tp"), None, None),
        P(("sp", "tp"), None, None),
    )
    out_specs = P(("sp", "tp"), None)
    return jax.shard_map(body, mesh=mesh, in_specs=in_specs, out_specs=out_specs, check_vma=False)
```

```python
import functools

import jax
import jax.numpy as jnp
from jax import lax
from jax.experimental import pallas as pl
from jax.experimental.pallas import tpu as pltpu
from jax.sharding import PartitionSpec as P

GROUPS = 4
CAPACITY = 6
STRIDE = 101
INVERSE = 109
RING = 4
PARTS = 8
BATCH = 16
FIRST_WINDOW = 2

norm_eps = 1e-05
clamp_limit = 7.0
sigmoid_alpha = 1.702
MESH = pl.DeviceIdType.MESH
F32 = jnp.float32
BF16 = jnp.bfloat16


def iota(shape, axis):
    return lax.broadcasted_iota(jnp.int32, shape, axis)


def quotient(value, divisor):
    return jnp.floor((value.astype(F32) + 0.5) * (1.0 / divisor))


def dot(left, right):
    return jnp.dot(left, right, preferred_element_type=F32)


def layer_kernel(
    stream_hbm,
    projected_hbm,
    segments_hbm,
    group_hbm,
    scale_hbm,
    out_weight_hbm,
    gain_hbm,
    routes_hbm,
    weights_hbm,
    gate_hbm,
    up_hbm,
    down_hbm,
    combined_ref,
    stream_ref,
    extended,
    segments_ref,
    segments_before,
    group_ref,
    scale_ref,
    out_weight_ref,
    gain_ref,
    routes_ref,
    weights_ref,
    gate_ref,
    up_ref,
    down_ref,
    mixed_out,
    mixed_in,
    total,
    resid_ref,
    normed_ref,
    unpack_ref,
    pack_ref,
    rank_ref,
    rank_turned,
    share_turned,
    picks,
    wide_ref,
    tall_ref,
    hidden_ref,
    sent,
    arrived,
    results,
    returned,
    load_sems,
    halo_sems,
    mixed_sends,
    mixed_recvs,
    sent_sem,
    arrived_sems,
    results_sem,
    returned_sems,
    ready,
):
    sp_count, tp_count = lax.axis_size("sp"), lax.axis_size("tp")
    count = sp_count * tp_count
    sp, tp = lax.axis_index("sp"), lax.axis_index("tp")
    tokens, width = stream_ref.shape
    channels = width // tp_count
    group_width = width // GROUPS
    batches = count // BATCH
    rows = BATCH * CAPACITY
    piece = width // PARTS
    packed_rows = rows * PARTS
    message = CAPACITY * PARTS

    def peer_at(name, sign):
        step = lax.rem(name * STRIDE, count)
        sender = lax.rem(tp, 2) if sign > 0 else lax.rem(tp + step, 2)
        way = sign * (1 - 2 * sender)
        place = [
            lax.rem(index + way * part + RING, RING)
            for index, part in (
                (sp // RING, step // (2 * RING * RING)),
                (lax.rem(sp, RING), lax.rem(step // (2 * RING), RING)),
                (tp // 2, lax.rem(step // 2, RING)),
            )
        ]
        return (place[0] * RING + place[1], place[2] * 2 + lax.rem(tp + step, 2))

    loads = [
        pltpu.make_async_copy(source, target, load_sems.at[number])
        for number, (source, target) in enumerate(
            [
                (projected_hbm, extended.at[pl.ds(tokens, tokens * tp_count)]),
                (segments_hbm, segments_ref),
                (routes_hbm, routes_ref),
                (weights_hbm, weights_ref),
                (group_hbm, group_ref),
                (out_weight_hbm, out_weight_ref),
                (scale_hbm, scale_ref),
                (stream_hbm, stream_ref),
                (gain_hbm, gain_ref),
                (gate_hbm, gate_ref),
                (up_hbm, up_ref),
                (down_hbm, down_ref),
            ]
        )
    ]
    for load in loads:
        load.start()

    barrier = pltpu.get_barrier_semaphore()

    for step in range(1, tp_count):
        pl.semaphore_signal(
            barrier,
            inc=1,
            device_id=(sp, lax.rem(tp + step, tp_count)),
            device_id_type=MESH,
        )
    for step in range(1, sp_count):
        pl.semaphore_signal(
            barrier,
            inc=1,
            device_id=(lax.rem(sp + step, sp_count), tp),
            device_id_type=MESH,
        )

    turned = (packed_rows, packed_rows)

    def message_row(value):
        part = quotient(value, rows)
        within = value.astype(F32) - part * rows
        peer = quotient(within, CAPACITY)
        return peer * message + part * CAPACITY + (within - peer * CAPACITY)

    unpack_ref[...] = jnp.where(
        message_row(iota((packed_rows, 1), 0)) == iota(turned, 1).astype(F32), 1.0, 0.0
    ).astype(BF16)
    pack_ref[...] = jnp.where(
        message_row(iota((1, packed_rows), 1)) == iota(turned, 0).astype(F32), 1.0, 0.0
    ).astype(BF16)

    window = jnp.left_shift(FIRST_WINDOW, tp // (tp_count // GROUPS))
    extended[pl.ds(0, tokens - 16), :] = jnp.zeros((tokens - 16, channels), BF16)
    for load in loads[:2]:
        load.wait()
    back = tokens + iota((tokens, 2 * tokens), 0) - iota((tokens, 2 * tokens), 1)
    in_window = (back >= 0) & (back < window)

    def pool(block, docs_before):
        docs = segments_ref[block : block + 1, :]
        docs_there = jnp.concatenate([docs_before, docs], axis=1).astype(F32)
        docs_here = jnp.broadcast_to(docs.astype(F32), (tokens, tokens)).T
        docs_here = jnp.concatenate([docs_here, docs_here], axis=1)
        included = jnp.where(in_window & (docs_here == docs_there), 1.0, 0.0).astype(BF16)
        sums = dot(included, extended[pl.ds(block * tokens, 2 * tokens), :])
        counts = dot(included, jnp.ones((2 * tokens, channels), BF16))
        own = extended[pl.ds((block + 1) * tokens, tokens), :].astype(F32)
        mixed_out[block] = (sums / counts - own).astype(BF16)

    for block in range(1, tp_count):
        pool(block, segments_ref[block - 1 : block, :])

    pl.semaphore_wait(barrier, sp_count + tp_count - 2)

    following = (lax.rem(sp + 1, sp_count), tp)
    halo = [
        pltpu.make_async_remote_copy(
            extended.at[pl.ds(tokens * (tp_count + 1) - 16, 16)],
            extended.at[pl.ds(tokens - 16, 16)],
            halo_sems.at[0],
            halo_sems.at[1],
            device_id=following,
            device_id_type=MESH,
        ),
        pltpu.make_async_remote_copy(
            segments_ref,
            segments_before,
            halo_sems.at[2],
            halo_sems.at[3],
            device_id=following,
            device_id_type=MESH,
        ),
    ]
    for copy in halo:
        copy.start()

    def mixed_copy(peer):
        return pltpu.make_async_remote_copy(
            mixed_out.at[peer],
            mixed_in.at[tp],
            mixed_sends.at[peer],
            mixed_recvs.at[tp],
            device_id=(sp, peer),
            device_id_type=MESH,
        )

    for step in range(1, tp_count):
        peer = lax.rem(tp + step, tp_count)

        @pl.when(peer != 0)
        def _():
            mixed_copy(peer).start()

    for step in range(1, sp_count):
        pl.semaphore_signal(
            ready, inc=1, device_id=(lax.rem(sp + step, sp_count), tp), device_id_type=MESH
        )

    def packed():
        return dot(pack_ref[...], tall_ref[...]).astype(BF16).reshape(BATCH, message, piece)

    def unpack(block):
        tall = dot(unpack_ref[...], block.reshape(packed_rows, piece)).astype(BF16)
        for part in range(PARTS):
            wide_ref[:, part * piece : (part + 1) * piece] = tall[part * rows : (part + 1) * rows]

    for load in loads[2:4]:
        load.wait()
    named = routes_ref[...]
    offset = jnp.bitwise_and(named + tp, 1)
    way = 1 - 2 * lax.rem(tp, 2)
    for unit, own in ((2, tp // 2), (2 * RING, lax.rem(sp, RING)), (2 * RING * RING, sp // RING)):
        place = lax.shift_right_logical(named, unit.bit_length() - 1)
        offset = offset + jnp.bitwise_and((place - own) * way, RING - 1) * unit
    order = jnp.bitwise_and(offset * INVERSE, count - 1)
    square = (count, tokens)
    chosen = jnp.zeros(square, F32)
    share = jnp.zeros(square, F32)
    for choice in range(routes_ref.shape[0]):
        match = iota(square, 0) == order[choice : choice + 1, :]
        chosen = chosen + jnp.where(match, 1.0, 0.0)
        share = share + jnp.where(match, weights_ref[choice : choice + 1, :], 0.0)
    earlier = jnp.where(iota((tokens, tokens), 0) < iota((tokens, tokens), 1), 1.0, 0.0)
    rank = jnp.where(chosen > 0.0, dot(chosen.astype(BF16), earlier.astype(BF16)), -1.0)
    rank_ref[...] = rank.astype(BF16)
    rank_turned[...] = rank.T.astype(BF16)

    @pl.loop(0, batches)
    def _(batch):
        names = (batch * BATCH).astype(F32) + quotient(iota((rows, count), 0), CAPACITY)
        slot = iota((rows, 1), 0).astype(F32) - CAPACITY * quotient(iota((rows, 1), 0), CAPACITY)
        spread = jnp.where(names == iota((rows, count), 1).astype(F32), 1.0, 0.0).astype(BF16)
        picks[batch] = jnp.where(dot(spread, rank_ref[...]) == slot, 1.0, 0.0).astype(BF16)

    share = share.T
    share_high = share.astype(BF16)
    share_turned[0] = share_high
    share_turned[1] = (share - share_high.astype(F32)).astype(BF16)

    for copy in halo:
        copy.wait()
    docs_before = jnp.where(sp > 0, segments_before[tp_count - 1 : tp_count, :], -1)
    pool(0, docs_before)

    @pl.when(tp != 0)
    def _():
        mixed_copy(0).start()

    mixed_in[tp] = mixed_out[tp]

    for load in loads[4:9]:
        load.wait()
    total[...] = stream_ref[...].astype(F32)
    for step in (0, 1, 3, 2):
        per_group = tp_count // GROUPS
        group = lax.rem(tp // per_group + step, GROUPS)
        grouped = jnp.zeros((tokens, group_width), F32)
        for member in range(per_group):
            source = group * per_group + member

            @pl.when(source != tp)
            def _():
                block = mixed_in.at[source]
                pltpu.make_async_copy(block, block, mixed_recvs.at[source]).wait()

            grouped = grouped + dot(
                mixed_in[source], group_ref[group, member * channels : (member + 1) * channels, :]
            )
        scale = scale_ref[:, pl.ds(pl.multiple_of(group * group_width, group_width), group_width)]
        total[...] += dot((grouped * scale).astype(BF16), out_weight_ref[group])

    resid = total[...].astype(BF16)
    resid_ref[...] = resid
    values = resid.astype(F32)
    inverse = lax.rsqrt(jnp.mean(values * values, -1, keepdims=True) + norm_eps)
    normed_ref[...] = (values * inverse * gain_ref[...]).astype(BF16)

    pl.semaphore_wait(ready, sp_count - 1)

    @pl.loop(0, batches)
    def _(batch):
        select = picks[batch]
        for part in range(PARTS):
            tall_ref[part * rows : (part + 1) * rows, :] = dot(
                select, normed_ref[:, part * piece : (part + 1) * piece]
            ).astype(BF16)
        sent[pl.ds(batch * BATCH, BATCH)] = packed()

        @pl.when(batch == 0)
        def _():
            arrived[0] = sent[0]

        @pl.loop(jnp.where(batch == 0, 1, 0), BATCH)
        def _(step):
            name = batch * BATCH + step
            pltpu.make_async_remote_copy(
                sent.at[name],
                arrived.at[name],
                sent_sem,
                arrived_sems.at[batch],
                device_id=peer_at(name, 1),
                device_id_type=MESH,
            ).start()

    def wait_batch(buffer, sems, batch):
        @pl.when(batch == 0)
        def _():
            part = buffer.at[pl.ds(1, BATCH - 1)]
            pltpu.make_async_copy(part, part, sems.at[0]).wait()

        @pl.when(batch != 0)
        def _():
            part = buffer.at[pl.ds(batch * BATCH, BATCH)]
            pltpu.make_async_copy(part, part, sems.at[batch]).wait()

    for load in loads[9:]:
        load.wait()

    @pl.loop(0, batches)
    def _(batch):
        wait_batch(arrived, arrived_sems, batch)
        unpack(arrived[pl.ds(batch * BATCH, BATCH)])
        block = wide_ref[...]
        hidden = hidden_ref.shape[1]
        for start in range(0, hidden, 256):
            columns = slice(start, start + 256)
            gated = jnp.minimum(dot(block, gate_ref[0, :, columns]), clamp_limit)
            linear = jnp.clip(dot(block, up_ref[0, :, columns]), -clamp_limit, clamp_limit)
            hidden_ref[:, columns] = (
                gated * jax.nn.sigmoid(sigmoid_alpha * gated) * (linear + 1.0)
            ).astype(BF16)
        for part in range(PARTS):
            tall_ref[part * rows : (part + 1) * rows, :] = dot(
                hidden_ref[...], down_ref[0, :, part * piece : (part + 1) * piece]
            ).astype(BF16)
        results[pl.ds(batch * BATCH, BATCH)] = packed()

        @pl.when(batch == 0)
        def _():
            returned[0] = results[0]

        @pl.loop(jnp.where(batch == 0, 1, 0), BATCH)
        def _(step):
            name = batch * BATCH + step
            pltpu.make_async_remote_copy(
                results.at[name],
                returned.at[name],
                results_sem,
                returned_sems.at[batch],
                device_id=peer_at(name, -1),
                device_id_type=MESH,
            ).start()

    total[...] = resid_ref[...].astype(F32)

    @pl.loop(0, batches)
    def _(batch):
        names = (batch * BATCH).astype(F32) + quotient(iota((count, rows), 1), CAPACITY)
        slot = iota((1, rows), 1).astype(F32) - CAPACITY * quotient(iota((1, rows), 1), CAPACITY)
        spread = jnp.where(names == iota((count, rows), 0).astype(F32), 1.0, 0.0).astype(BF16)
        live = dot(rank_turned[...], spread) == slot
        high = jnp.where(live, dot(share_turned[0], spread), 0.0).astype(BF16)
        low = jnp.where(live, dot(share_turned[1], spread), 0.0).astype(BF16)
        wait_batch(returned, returned_sems, batch)
        unpack(returned[pl.ds(batch * BATCH, BATCH)])
        total[...] += dot(high, wide_ref[...]) + dot(low, wide_ref[...])

    combined_ref[...] = total[...].astype(BF16)

    for step in range(1, tp_count):
        mixed_copy(lax.rem(tp + step, tp_count)).wait_send()
    rest = pl.ds(1, count - 1)
    pltpu.make_async_copy(sent.at[rest], sent.at[rest], sent_sem).wait()
    pltpu.make_async_copy(results.at[rest], results.at[rest], results_sem).wait()


def body(
    stream,
    projected,
    segments,
    group_weight,
    group_scale,
    out_weight,
    ffn_gain,
    routes,
    route_weights,
    expert_gate,
    expert_up,
    expert_down,
):
    tokens, width = stream.shape
    tp_count = lax.axis_size("tp")
    count = lax.axis_size("sp") * tp_count
    channels = width // tp_count
    hidden = expert_gate.shape[2]
    rows = BATCH * CAPACITY
    piece = width // PARTS
    operands = (
        stream,
        projected,
        segments.reshape(-1, tokens),
        group_weight,
        group_scale.reshape(1, -1),
        out_weight.reshape(GROUPS, width // GROUPS, width),
        ffn_gain.reshape(1, -1),
        routes.T,
        route_weights.T,
        expert_gate,
        expert_up,
        expert_down,
    )
    messages = (count, CAPACITY * PARTS, piece)
    batches = count // BATCH
    vmem = pltpu.VMEM
    dma = pltpu.SemaphoreType.DMA
    return pl.pallas_call(
        layer_kernel,
        out_shape=jax.ShapeDtypeStruct((tokens, width), BF16),
        in_specs=[pl.BlockSpec(memory_space=pltpu.MemorySpace.HBM)] * len(operands),
        out_specs=pl.BlockSpec(memory_space=pltpu.VMEM),
        scratch_shapes=[
            vmem((tokens, width), BF16),
            vmem((tokens * (tp_count + 1), channels), BF16),
            vmem((tp_count, tokens), jnp.int32),
            vmem((tp_count, tokens), jnp.int32),
            vmem(group_weight.shape, BF16),
            vmem((1, width), F32),
            vmem((GROUPS, width // GROUPS, width), BF16),
            vmem((1, width), F32),
            vmem(routes.shape[::-1], jnp.int32),
            vmem(routes.shape[::-1], F32),
            vmem(expert_gate.shape, BF16),
            vmem(expert_up.shape, BF16),
            vmem(expert_down.shape, BF16),
            vmem((tp_count, tokens, channels), BF16),
            vmem((tp_count, tokens, channels), BF16),
            vmem((tokens, width), F32),
            vmem((tokens, width), BF16),
            vmem((tokens, width), BF16),
            vmem((rows * PARTS, rows * PARTS), BF16),
            vmem((rows * PARTS, rows * PARTS), BF16),
            vmem((count, tokens), BF16),
            vmem((tokens, count), BF16),
            vmem((2, tokens, count), BF16),
            vmem((batches, rows, tokens), BF16),
            vmem((rows, width), BF16),
            vmem((rows * PARTS, piece), BF16),
            vmem((rows, hidden), BF16),
            vmem(messages, BF16),
            vmem(messages, BF16),
            vmem(messages, BF16),
            vmem(messages, BF16),
            dma((len(operands),)),
            dma((4,)),
            dma((tp_count,)),
            dma((tp_count,)),
            dma,
            dma((batches,)),
            dma,
            dma((batches,)),
            pltpu.SemaphoreType.REGULAR,
        ],
        name="layer",
        compiler_params=pltpu.CompilerParams(
            collective_id=0, has_side_effects=True, vmem_limit_bytes=50 << 20
        ),
    )(*(pltpu.with_memory_space_constraint(operand, pltpu.MemorySpace.HBM) for operand in operands))


def solution(mesh):
    in_specs = (
        P(("sp", "tp"), None),
        P("sp", "tp"),
        P("sp"),
        P(),
        P(),
        P(),
        P(),
        P(("sp", "tp"), None),
        P(("sp", "tp"), None),
        P(("sp", "tp"), None, None),
        P(("sp", "tp"), None, None),
        P(("sp", "tp"), None, None),
    )
    out_specs = P(("sp", "tp"), None)
    return jax.shard_map(body, mesh=mesh, in_specs=in_specs, out_specs=out_specs, check_vma=False)
```

```python
import functools

import jax
import jax.numpy as jnp
from jax import lax
from jax.experimental import pallas as pl
from jax.experimental.pallas import tpu as pltpu
from jax.sharding import PartitionSpec as P

GROUPS = 4
CAPACITY = 6
STRIDE = 101
INVERSE = 109
RING = 4
PARTS = 8
BATCH = 16
FIRST_WINDOW = 2

norm_eps = 1e-05
clamp_limit = 7.0
sigmoid_alpha = 1.702
MESH = pl.DeviceIdType.MESH
F32 = jnp.float32
BF16 = jnp.bfloat16


def iota(shape, axis):
    return lax.broadcasted_iota(jnp.int32, shape, axis)


def quotient(value, divisor):
    return jnp.floor((value.astype(F32) + 0.5) * (1.0 / divisor))


def dot(left, right):
    return jnp.dot(left, right, preferred_element_type=F32)


def layer_kernel(
    stream_hbm,
    projected_hbm,
    segments_hbm,
    group_hbm,
    scale_hbm,
    out_weight_hbm,
    gain_hbm,
    routes_hbm,
    weights_hbm,
    gate_hbm,
    up_hbm,
    down_hbm,
    combined_ref,
    stream_ref,
    extended,
    segments_ref,
    segments_before,
    group_ref,
    scale_ref,
    out_weight_ref,
    gain_ref,
    routes_ref,
    weights_ref,
    gate_ref,
    up_ref,
    down_ref,
    mixed_out,
    mixed_in,
    total,
    resid_ref,
    normed_ref,
    unpack_ref,
    pack_ref,
    rank_ref,
    rank_turned,
    share_turned,
    picks,
    wide_ref,
    tall_ref,
    hidden_ref,
    sent,
    arrived,
    results,
    returned,
    load_sems,
    halo_sems,
    mixed_sends,
    mixed_recvs,
    sent_sem,
    arrived_sems,
    results_sem,
    returned_sems,
    ready,
):
    sp_count, tp_count = lax.axis_size("sp"), lax.axis_size("tp")
    count = sp_count * tp_count
    sp, tp = lax.axis_index("sp"), lax.axis_index("tp")
    tokens, width = stream_ref.shape
    channels = width // tp_count
    group_width = width // GROUPS
    batches = count // BATCH
    rows = BATCH * CAPACITY
    piece = width // PARTS
    packed_rows = rows * PARTS
    message = CAPACITY * PARTS

    def peer_at(name, sign):
        step = lax.rem(name * STRIDE, count)
        sender = lax.rem(tp, 2) if sign > 0 else lax.rem(tp + step, 2)
        way = sign * (1 - 2 * sender)
        place = [
            lax.rem(index + way * part + RING, RING)
            for index, part in (
                (sp // RING, step // (2 * RING * RING)),
                (lax.rem(sp, RING), lax.rem(step // (2 * RING), RING)),
                (tp // 2, lax.rem(step // 2, RING)),
            )
        ]
        return (place[0] * RING + place[1], place[2] * 2 + lax.rem(tp + step, 2))

    loads = [
        pltpu.make_async_copy(source, target, load_sems.at[number])
        for number, (source, target) in enumerate(
            [
                (projected_hbm, extended.at[pl.ds(tokens, tokens * tp_count)]),
                (segments_hbm, segments_ref),
                (routes_hbm, routes_ref),
                (weights_hbm, weights_ref),
                (group_hbm, group_ref),
                (out_weight_hbm, out_weight_ref),
                (scale_hbm, scale_ref),
                (stream_hbm, stream_ref),
                (gain_hbm, gain_ref),
                (gate_hbm, gate_ref),
                (up_hbm, up_ref),
                (down_hbm, down_ref),
            ]
        )
    ]
    for load in loads:
        load.start()

    barrier = pltpu.get_barrier_semaphore()

    for step in range(1, tp_count):
        pl.semaphore_signal(
            barrier,
            inc=1,
            device_id=(sp, lax.rem(tp + step, tp_count)),
            device_id_type=MESH,
        )
    for step in range(1, sp_count):
        pl.semaphore_signal(
            barrier,
            inc=1,
            device_id=(lax.rem(sp + step, sp_count), tp),
            device_id_type=MESH,
        )

    turned = (packed_rows, packed_rows)

    def message_row(value):
        part = quotient(value, rows)
        within = value.astype(F32) - part * rows
        peer = quotient(within, CAPACITY)
        return peer * message + part * CAPACITY + (within - peer * CAPACITY)

    unpack_ref[...] = jnp.where(
        message_row(iota((packed_rows, 1), 0)) == iota(turned, 1).astype(F32), 1.0, 0.0
    ).astype(BF16)
    pack_ref[...] = jnp.where(
        message_row(iota((1, packed_rows), 1)) == iota(turned, 0).astype(F32), 1.0, 0.0
    ).astype(BF16)

    window = jnp.left_shift(FIRST_WINDOW, tp // (tp_count // GROUPS))
    extended[pl.ds(0, tokens - 16), :] = jnp.zeros((tokens - 16, channels), BF16)
    for load in loads[:2]:
        load.wait()
    back = tokens + iota((tokens, 2 * tokens), 0) - iota((tokens, 2 * tokens), 1)
    in_window = (back >= 0) & (back < window)

    def pool(block, docs_before):
        docs = segments_ref[block : block + 1, :]
        docs_there = jnp.concatenate([docs_before, docs], axis=1).astype(F32)
        docs_here = jnp.broadcast_to(docs.astype(F32), (tokens, tokens)).T
        docs_here = jnp.concatenate([docs_here, docs_here], axis=1)
        included = jnp.where(in_window & (docs_here == docs_there), 1.0, 0.0).astype(BF16)
        sums = dot(included, extended[pl.ds(block * tokens, 2 * tokens), :])
        counts = dot(included, jnp.ones((2 * tokens, channels), BF16))
        own = extended[pl.ds((block + 1) * tokens, tokens), :].astype(F32)
        mixed_out[block] = (sums / counts - own).astype(BF16)

    for block in range(1, tp_count):
        pool(block, segments_ref[block - 1 : block, :])

    pl.semaphore_wait(barrier, sp_count + tp_count - 2)

    following = (lax.rem(sp + 1, sp_count), tp)
    halo = [
        pltpu.make_async_remote_copy(
            extended.at[pl.ds(tokens * (tp_count + 1) - 16, 16)],
            extended.at[pl.ds(tokens - 16, 16)],
            halo_sems.at[0],
            halo_sems.at[1],
            device_id=following,
            device_id_type=MESH,
        ),
        pltpu.make_async_remote_copy(
            segments_ref,
            segments_before,
            halo_sems.at[2],
            halo_sems.at[3],
            device_id=following,
            device_id_type=MESH,
        ),
    ]
    for copy in halo:
        copy.start()

    def mixed_copy(peer):
        return pltpu.make_async_remote_copy(
            mixed_out.at[peer],
            mixed_in.at[tp],
            mixed_sends.at[peer],
            mixed_recvs.at[tp],
            device_id=(sp, peer),
            device_id_type=MESH,
        )

    for step in range(1, tp_count):
        peer = lax.rem(tp + step, tp_count)

        @pl.when(peer != 0)
        def _():
            mixed_copy(peer).start()

    for step in range(1, sp_count):
        pl.semaphore_signal(
            ready, inc=1, device_id=(lax.rem(sp + step, sp_count), tp), device_id_type=MESH
        )

    def packed(half):
        chosen_rows = pack_ref[half * packed_rows // 2 : (half + 1) * packed_rows // 2, :]
        return dot(chosen_rows, tall_ref[...]).astype(BF16).reshape(BATCH // 2, message, piece)

    def unpack(block):
        tall = dot(unpack_ref[...], block.reshape(packed_rows, piece)).astype(BF16)
        for part in range(PARTS):
            wide_ref[:, part * piece : (part + 1) * piece] = tall[part * rows : (part + 1) * rows]

    for load in loads[2:4]:
        load.wait()
    named = routes_ref[...]
    offset = jnp.bitwise_and(named + tp, 1)
    way = 1 - 2 * lax.rem(tp, 2)
    for unit, own in ((2, tp // 2), (2 * RING, lax.rem(sp, RING)), (2 * RING * RING, sp // RING)):
        place = lax.shift_right_logical(named, unit.bit_length() - 1)
        offset = offset + jnp.bitwise_and((place - own) * way, RING - 1) * unit
    order = jnp.bitwise_and(offset * INVERSE, count - 1)
    square = (count, tokens)
    chosen = jnp.zeros(square, F32)
    share = jnp.zeros(square, F32)
    for choice in range(routes_ref.shape[0]):
        match = iota(square, 0) == order[choice : choice + 1, :]
        chosen = chosen + jnp.where(match, 1.0, 0.0)
        share = share + jnp.where(match, weights_ref[choice : choice + 1, :], 0.0)
    earlier = jnp.where(iota((tokens, tokens), 0) < iota((tokens, tokens), 1), 1.0, 0.0)
    rank = jnp.where(chosen > 0.0, dot(chosen.astype(BF16), earlier.astype(BF16)), -1.0)
    rank_ref[...] = rank.astype(BF16)
    rank_turned[...] = rank.T.astype(BF16)

    @pl.loop(0, batches)
    def _(batch):
        names = (batch * BATCH).astype(F32) + quotient(iota((rows, count), 0), CAPACITY)
        slot = iota((rows, 1), 0).astype(F32) - CAPACITY * quotient(iota((rows, 1), 0), CAPACITY)
        spread = jnp.where(names == iota((rows, count), 1).astype(F32), 1.0, 0.0).astype(BF16)
        picks[batch] = jnp.where(dot(spread, rank_ref[...]) == slot, 1.0, 0.0).astype(BF16)

    share = share.T
    share_high = share.astype(BF16)
    share_turned[0] = share_high
    share_turned[1] = (share - share_high.astype(F32)).astype(BF16)

    for copy in halo:
        copy.wait()
    docs_before = jnp.where(sp > 0, segments_before[tp_count - 1 : tp_count, :], -1)
    pool(0, docs_before)

    @pl.when(tp != 0)
    def _():
        mixed_copy(0).start()

    mixed_in[tp] = mixed_out[tp]

    for load in loads[4:9]:
        load.wait()
    total[...] = stream_ref[...].astype(F32)
    for step in (0, 1, 3, 2):
        per_group = tp_count // GROUPS
        group = lax.rem(tp // per_group + step, GROUPS)
        grouped = jnp.zeros((tokens, group_width), F32)
        for member in range(per_group):
            source = group * per_group + member

            @pl.when(source != tp)
            def _():
                block = mixed_in.at[source]
                pltpu.make_async_copy(block, block, mixed_recvs.at[source]).wait()

            grouped = grouped + dot(
                mixed_in[source], group_ref[group, member * channels : (member + 1) * channels, :]
            )
        scale = scale_ref[:, pl.ds(pl.multiple_of(group * group_width, group_width), group_width)]
        total[...] += dot((grouped * scale).astype(BF16), out_weight_ref[group])

    resid = total[...].astype(BF16)
    resid_ref[...] = resid
    values = resid.astype(F32)
    inverse = lax.rsqrt(jnp.mean(values * values, -1, keepdims=True) + norm_eps)
    normed_ref[...] = (values * inverse * gain_ref[...]).astype(BF16)

    pl.semaphore_wait(ready, sp_count - 1)

    @pl.loop(0, batches)
    def _(batch):
        select = picks[batch]
        for part in range(PARTS):
            tall_ref[part * rows : (part + 1) * rows, :] = dot(
                select, normed_ref[:, part * piece : (part + 1) * piece]
            ).astype(BF16)
        for half in range(2):
            sent[pl.ds(batch * BATCH + half * BATCH // 2, BATCH // 2)] = packed(half)

            if half == 0:

                @pl.when(batch == 0)
                def _():
                    arrived[0] = sent[0]

            @pl.loop(jnp.where(batch == 0, 1 - half, 0), BATCH // 2)
            def _(step):
                name = batch * BATCH + half * BATCH // 2 + step
                pltpu.make_async_remote_copy(
                    sent.at[name],
                    arrived.at[name],
                    sent_sem,
                    arrived_sems.at[batch],
                    device_id=peer_at(name, 1),
                    device_id_type=MESH,
                ).start()

    def wait_batch(buffer, sems, batch):
        @pl.when(batch == 0)
        def _():
            part = buffer.at[pl.ds(1, BATCH - 1)]
            pltpu.make_async_copy(part, part, sems.at[0]).wait()

        @pl.when(batch != 0)
        def _():
            part = buffer.at[pl.ds(batch * BATCH, BATCH)]
            pltpu.make_async_copy(part, part, sems.at[batch]).wait()

    for load in loads[9:]:
        load.wait()

    @pl.loop(0, batches)
    def _(batch):
        wait_batch(arrived, arrived_sems, batch)
        unpack(arrived[pl.ds(batch * BATCH, BATCH)])
        block = wide_ref[...]
        hidden = hidden_ref.shape[1]
        for start in range(0, hidden, 256):
            columns = slice(start, start + 256)
            gated = jnp.minimum(dot(block, gate_ref[0, :, columns]), clamp_limit)
            linear = jnp.clip(dot(block, up_ref[0, :, columns]), -clamp_limit, clamp_limit)
            hidden_ref[:, columns] = (
                gated * jax.nn.sigmoid(sigmoid_alpha * gated) * (linear + 1.0)
            ).astype(BF16)
        for part in range(PARTS):
            tall_ref[part * rows : (part + 1) * rows, :] = dot(
                hidden_ref[...], down_ref[0, :, part * piece : (part + 1) * piece]
            ).astype(BF16)
        for half in range(2):
            results[pl.ds(batch * BATCH + half * BATCH // 2, BATCH // 2)] = packed(half)

            if half == 0:

                @pl.when(batch == 0)
                def _():
                    returned[0] = results[0]

            @pl.loop(jnp.where(batch == 0, 1 - half, 0), BATCH // 2)
            def _(step):
                name = batch * BATCH + half * BATCH // 2 + step
                pltpu.make_async_remote_copy(
                    results.at[name],
                    returned.at[name],
                    results_sem,
                    returned_sems.at[batch],
                    device_id=peer_at(name, -1),
                    device_id_type=MESH,
                ).start()

    total[...] = resid_ref[...].astype(F32)

    @pl.loop(0, batches)
    def _(batch):
        names = (batch * BATCH).astype(F32) + quotient(iota((count, rows), 1), CAPACITY)
        slot = iota((1, rows), 1).astype(F32) - CAPACITY * quotient(iota((1, rows), 1), CAPACITY)
        spread = jnp.where(names == iota((count, rows), 0).astype(F32), 1.0, 0.0).astype(BF16)
        live = dot(rank_turned[...], spread) == slot
        high = jnp.where(live, dot(share_turned[0], spread), 0.0).astype(BF16)
        low = jnp.where(live, dot(share_turned[1], spread), 0.0).astype(BF16)
        wait_batch(returned, returned_sems, batch)
        unpack(returned[pl.ds(batch * BATCH, BATCH)])
        total[...] += dot(high, wide_ref[...]) + dot(low, wide_ref[...])

    combined_ref[...] = total[...].astype(BF16)

    for step in range(1, tp_count):
        mixed_copy(lax.rem(tp + step, tp_count)).wait_send()
    rest = pl.ds(1, count - 1)
    pltpu.make_async_copy(sent.at[rest], sent.at[rest], sent_sem).wait()
    pltpu.make_async_copy(results.at[rest], results.at[rest], results_sem).wait()


def body(
    stream,
    projected,
    segments,
    group_weight,
    group_scale,
    out_weight,
    ffn_gain,
    routes,
    route_weights,
    expert_gate,
    expert_up,
    expert_down,
):
    tokens, width = stream.shape
    tp_count = lax.axis_size("tp")
    count = lax.axis_size("sp") * tp_count
    channels = width // tp_count
    hidden = expert_gate.shape[2]
    rows = BATCH * CAPACITY
    piece = width // PARTS
    operands = (
        stream,
        projected,
        segments.reshape(-1, tokens),
        group_weight,
        group_scale.reshape(1, -1),
        out_weight.reshape(GROUPS, width // GROUPS, width),
        ffn_gain.reshape(1, -1),
        routes.T,
        route_weights.T,
        expert_gate,
        expert_up,
        expert_down,
    )
    messages = (count, CAPACITY * PARTS, piece)
    batches = count // BATCH
    vmem = pltpu.VMEM
    dma = pltpu.SemaphoreType.DMA
    return pl.pallas_call(
        layer_kernel,
        out_shape=jax.ShapeDtypeStruct((tokens, width), BF16),
        in_specs=[pl.BlockSpec(memory_space=pltpu.MemorySpace.HBM)] * len(operands),
        out_specs=pl.BlockSpec(memory_space=pltpu.VMEM),
        scratch_shapes=[
            vmem((tokens, width), BF16),
            vmem((tokens * (tp_count + 1), channels), BF16),
            vmem((tp_count, tokens), jnp.int32),
            vmem((tp_count, tokens), jnp.int32),
            vmem(group_weight.shape, BF16),
            vmem((1, width), F32),
            vmem((GROUPS, width // GROUPS, width), BF16),
            vmem((1, width), F32),
            vmem(routes.shape[::-1], jnp.int32),
            vmem(routes.shape[::-1], F32),
            vmem(expert_gate.shape, BF16),
            vmem(expert_up.shape, BF16),
            vmem(expert_down.shape, BF16),
            vmem((tp_count, tokens, channels), BF16),
            vmem((tp_count, tokens, channels), BF16),
            vmem((tokens, width), F32),
            vmem((tokens, width), BF16),
            vmem((tokens, width), BF16),
            vmem((rows * PARTS, rows * PARTS), BF16),
            vmem((rows * PARTS, rows * PARTS), BF16),
            vmem((count, tokens), BF16),
            vmem((tokens, count), BF16),
            vmem((2, tokens, count), BF16),
            vmem((batches, rows, tokens), BF16),
            vmem((rows, width), BF16),
            vmem((rows * PARTS, piece), BF16),
            vmem((rows, hidden), BF16),
            vmem(messages, BF16),
            vmem(messages, BF16),
            vmem(messages, BF16),
            vmem(messages, BF16),
            dma((len(operands),)),
            dma((4,)),
            dma((tp_count,)),
            dma((tp_count,)),
            dma,
            dma((batches,)),
            dma,
            dma((batches,)),
            pltpu.SemaphoreType.REGULAR,
        ],
        name="layer",
        compiler_params=pltpu.CompilerParams(
            collective_id=0, has_side_effects=True, vmem_limit_bytes=50 << 20
        ),
    )(*(pltpu.with_memory_space_constraint(operand, pltpu.MemorySpace.HBM) for operand in operands))


def solution(mesh):
    in_specs = (
        P(("sp", "tp"), None),
        P("sp", "tp"),
        P("sp"),
        P(),
        P(),
        P(),
        P(),
        P(("sp", "tp"), None),
        P(("sp", "tp"), None),
        P(("sp", "tp"), None, None),
        P(("sp", "tp"), None, None),
        P(("sp", "tp"), None, None),
    )
    out_specs = P(("sp", "tp"), None)
    return jax.shard_map(body, mesh=mesh, in_specs=in_specs, out_specs=out_specs, check_vma=False)
```
